32 devices in a mesh: row: 8 (over z, core), col: 4 (over y, x).
Axes of the slice: x: 2, y: 2, z: 4, core: 2. Of those that a mesh axis runs over, the one named last changes fastest.
Arguments:
- tokens: bfloat16 [4096, 4096], P('row', 'col'), may hold values from -6 to 6
- norm_gain: float32 [4096], replicated, may hold values from 0.1 to 1.9
- out_weight: bfloat16 [4096, 4096], P(None, 'col'), may hold values from -0.09375 to 0.09375
Outputs:
- mixed: bfloat16 [4096, 4096], P('row', 'col')
The draws below stay inside these ranges and needn't reach their ends.
All inputs are finite; a program needn't handle non-finite values.
Results may differ from the reference program's by a relative error of at most 0.015.
Values may be sent and summed in bfloat16 or wider, within the bound.
No kernel may reach another device: no remote copies, remote signals or barrier semaphores. Data moves between devices by JAX's collectives and lax.ppermute only.
A program may use at most 64 MiB of HBM per device.

```python
import jax
import jax.numpy as jnp
from jax import lax

D = 4096
GROUPS = 4
CG = 1024
SEQ = 4096


def block_levels(key, shape, shards, low, high):
    def one(position, shards_of):
        heights = jax.random.uniform(jax.random.fold_in(jax.random.fold_in(key, 6), position), (shards_of,), jnp.float32, low / len(shards), high / len(shards))
        return jnp.repeat(jnp.exp(heights), shape[position] // shards_of).reshape((-1,) + (1,) * (len(shape) - position - 1))

    level = one(*shards[0])
    for cut in shards[1:]:
        level = level * one(*cut)
    return level


def scatter_about(own_key, dims, width, reach, cuts=(), held_as=jnp.bfloat16):
    result = jax.random.normal(own_key, dims, jnp.float32) * width
    if len(cuts) > 0:
        result = block_levels(own_key, dims, cuts, -0.22, 0.18) * result
    return jnp.clip(result, min=-reach, max=reach).astype(held_as)


def setup_inputs(seed: int = 0) -> dict:
    key_of = jax.random.split(jax.random.key(seed), 4)
    return {
        "tokens": scatter_about(key_of[0], (SEQ, D), 1.0, 6.0, ((0, 8), (1, 4))),
        "norm_gain": jnp.clip(1.0 + 0.18 * jax.random.normal(key_of[1], (D,), jnp.float32), 0.1, 1.9),
        "out_weight": scatter_about(key_of[2], (D, D), D ** -0.5, 0.09375, ((1, 4),)),
    }


def reference(tokens, norm_gain, out_weight):
    values = tokens.astype(jnp.float32)
    inv_rms = lax.rsqrt(lax.optimization_barrier(jnp.mean(values * values, axis=-1, keepdims=True)) + 1e-06)
    normed = lax.optimization_barrier((values * inv_rms * norm_gain).astype(jnp.bfloat16))
    grouped = normed.astype(jnp.float32).reshape(SEQ, GROUPS, CG)
    spectrum = jnp.fft.fftn(grouped, axes=(0, 2), norm='ortho').real
    mixed_in = spectrum.reshape(SEQ, D).astype(jnp.bfloat16)
    return jnp.dot(mixed_in, out_weight, preferred_element_type=jnp.float32).astype(jnp.bfloat16)
```

```python
import math

import jax
import jax.numpy as jnp
from jax import lax
from jax.sharding import PartitionSpec as P

GROUPS = 4


EPSILON = 1e-06
PRECISE = lax.Precision.HIGHEST


def phases(left_idx, right_idx, period):
    product = left_idx[:, None] * right_idx[None, :] % period
    angles = product.astype(jnp.float32) * (2.0 * math.pi / period)
    return (jnp.cos(angles), jnp.sin(angles))


def split_table(table):
    table_high = table.astype(jnp.bfloat16)
    remainder = table - table_high.astype(jnp.float32)
    table_middle = remainder.astype(jnp.bfloat16)
    table_low = (remainder - table_middle.astype(jnp.float32)).astype(jnp.bfloat16)
    return (table_high, table_middle, table_low)


def on_device(tokens, norm_gain, out_weight):
    row_count = lax.axis_size("row")
    col_count = lax.axis_size("col")
    block_len, local_width = tokens.shape
    full_width = local_width * col_count
    group_len = full_width // GROUPS
    share_len = block_len // col_count
    seq_len = block_len * row_count
    slab_len = full_width // row_count
    col_index = lax.axis_index("col")
    chan_idx = jnp.arange(group_len, dtype=jnp.int32)
    cosines, sines = phases(chan_idx, chan_idx, group_len)
    chan_table = jnp.concatenate([cosines, sines], axis=1) / math.sqrt(group_len)
    table_parts = split_table(chan_table)
    arranged = tokens.reshape(col_count, share_len, local_width)
    portion = lax.all_to_all(arranged, "col", split_axis=0, concat_axis=2, tiled=True)
    item_count = portion.shape[1]
    values = portion.astype(jnp.float32)
    inv_rms = lax.rsqrt(jnp.mean(values * values, axis=-1, keepdims=True) + EPSILON)
    normed = lax.optimization_barrier((values * inv_rms * norm_gain).astype(jnp.bfloat16))
    grouped = normed.reshape(item_count, GROUPS, group_len)
    result = jnp.einsum("pgm,mj->pgj", grouped, table_parts[0], preferred_element_type=jnp.float32)
    result = result + jnp.einsum(
        "pgm,mj->pgj", grouped, table_parts[1], preferred_element_type=jnp.float32
    )
    result = result + jnp.einsum(
        "pgm,mj->pgj", grouped, table_parts[2], preferred_element_type=jnp.float32
    )
    high_idx = jnp.arange(row_count, dtype=jnp.int32)
    high_cos, high_sin = phases(high_idx, high_idx, row_count)
    high_table = jnp.concatenate(
        [jnp.concatenate([high_cos, -high_sin], 1), jnp.concatenate([-high_sin, -high_cos], 1)], 0
    )
    parts = (
        lax.all_to_all(
            result[..., :group_len].reshape(1, item_count, full_width),
            "row",
            split_axis=2,
            concat_axis=0,
            tiled=True,
        ),
        lax.all_to_all(
            result[..., group_len:].reshape(1, item_count, full_width),
            "row",
            split_axis=2,
            concat_axis=0,
            tiled=True,
        ),
    )
    item_count = parts[0].shape[1]
    stacked = jnp.concatenate(parts, 0).reshape(2 * row_count, item_count * slab_len)
    result = jnp.dot(high_table, stacked, precision=PRECISE)
    real_part = result[:row_count].reshape(row_count, item_count, slab_len)
    imag_part = result[row_count:].reshape(row_count, item_count, slab_len)
    local_pos = col_index * share_len + jnp.arange(share_len, dtype=jnp.int32)
    twist_cos, twist_sin = phases(high_idx, local_pos, seq_len)
    twist_cos = twist_cos[:, :, None]
    twist_sin = twist_sin[:, :, None]
    turned_real = real_part * twist_cos + imag_part * twist_sin
    turned_imag = imag_part * twist_cos - real_part * twist_sin
    low_idx = jnp.arange(block_len, dtype=jnp.int32)
    low_cos, low_sin = phases(low_idx, low_idx, block_len)
    low_cos = low_cos / math.sqrt(seq_len)
    low_sin = low_sin / math.sqrt(seq_len)
    low_table = jnp.concatenate([low_cos, low_sin], 1)
    stacked = jnp.concatenate(
        (
            lax.all_to_all(turned_real, "col", split_axis=0, concat_axis=1, tiled=True),
            lax.all_to_all(turned_imag, "col", split_axis=0, concat_axis=1, tiled=True),
        ),
        1,
    )
    finished = (jnp.einsum("ks,asc->akc", low_table, stacked, precision=PRECISE),)[0]
    spectrum = finished.astype(jnp.bfloat16)
    returned = lax.all_to_all(spectrum, "row", split_axis=1, concat_axis=2, tiled=True)
    mapped = jnp.einsum(
        "akd,de->kae",
        lax.all_gather(returned, "col", axis=0, tiled=True),
        out_weight,
        preferred_element_type=jnp.float32,
    )
    return mapped.astype(jnp.bfloat16).reshape(block_len, local_width)


def cosines_of(product, period, phase=0.0):
    return jnp.cos((product % period).astype(jnp.float32) * (2.0 * math.pi / period) - phase)


def channel_table(row_count, width):
    slab = width // row_count
    half = slab // 2
    coarse_len = 1 << (width.bit_length() // 2)
    lane = jnp.arange(width, dtype=jnp.int32)
    in_slab = lane % slab
    freq = (lane // slab) * half + in_slab % half
    is_sine = in_slab >= half
    packed = is_sine & (freq == 0)
    freq = jnp.where(packed, width // 2, freq)[None, :]
    quarter = jnp.where(is_sine & ~packed, 0.5 * math.pi, 0.0)[None, :]
    coarse = jnp.arange(0, width, coarse_len, dtype=jnp.int32)[:, None]
    fine = jnp.arange(coarse_len, dtype=jnp.int32)[:, None]
    scale = 1.0 / math.sqrt(width)
    coarse_cos = cosines_of(coarse * freq, width)
    coarse_sin = cosines_of(coarse * freq, width, 0.5 * math.pi)
    fine_cos = cosines_of(fine * freq, width, quarter) * scale
    fine_sin = cosines_of(fine * freq, width, quarter + 0.5 * math.pi) * scale
    table = (
        coarse_cos[:, None, :] * fine_cos[None] - coarse_sin[:, None, :] * fine_sin[None]
    )
    return table.astype(jnp.bfloat16).reshape(width, width)


def folding_matrix(row_index, row_count, width):
    slab = width // row_count
    half = slab // 2
    out_idx = jnp.arange(width, dtype=jnp.int32)[:, None]
    source = (row_index - out_idx // slab) % row_count
    in_slab = out_idx % slab
    freq = source * half + in_slab % half
    is_sine = in_slab >= half
    packed = is_sine & (freq == 0)
    freq = jnp.where(packed, width // 2, freq)
    sign = jnp.where(is_sine & ~packed, -1.0, 1.0)
    chan = jnp.arange(width, dtype=jnp.int32)[None, :]
    straight = jnp.where(chan == freq, sign, 0.0)
    mirrored = jnp.where((chan == (width - freq) % width) & (chan != freq), 1.0, 0.0)
    return (straight + mirrored).astype(jnp.bfloat16)


def on_device_whole_groups(tokens, norm_gain, out_weight):
    row_count = lax.axis_size("row")
    col_count = lax.axis_size("col")
    block_len, width = tokens.shape
    full_width = width * col_count
    slab = width // row_count
    half = slab // 2
    seq_len = block_len * row_count
    low_len = block_len // row_count
    row_index = lax.axis_index("row")
    col_index = lax.axis_index("col")

    def across_col(value, flip):
        return lax.ppermute(value, "col", [(k, k ^ flip) for k in range(col_count)])

    def along_row(value, shift):
        return lax.ppermute(
            value, "row", [(k, (k + shift) % row_count) for k in range(row_count)]
        )

    values = tokens.astype(jnp.float32)
    squares = jnp.sum(values * values, axis=-1)
    total = squares
    for flip in range(1, col_count):
        total = total + across_col(squares, flip)
    inv_rms = lax.rsqrt(total / full_width + EPSILON)
    gain = lax.dynamic_slice(norm_gain, (col_index * width,), (width,))
    gained = (values * gain).astype(jnp.bfloat16)
    chan = jnp.dot(gained, channel_table(row_count, width), preferred_element_type=jnp.float32)
    chan = (chan * inv_rms[:, None]).astype(jnp.bfloat16)
    chan = chan.reshape(block_len, row_count, slab).transpose(1, 0, 2)

    def to_row(blocks, shift):
        return lax.dynamic_index_in_dim(blocks, (row_index + shift) % row_count, 0, keepdims=False)

    got = [to_row(chan, 0)]
    for shift in range(1, row_count):
        got.append(along_row(to_row(chan, shift), shift))

    wide = [value.astype(jnp.float32) for value in got]
    local_pos = row_index * block_len + jnp.arange(block_len, dtype=jnp.int32)
    lane = jnp.arange(slab, dtype=jnp.int32)
    takes_sine = (lane >= half) & ~((lane == half) & (row_index == 0))
    reals, imags = [], []
    for high in range(row_count):
        part_cos = 0.0
        part_sin = 0.0
        for shift in range(row_count):
            angle = 2.0 * math.pi * (shift * high % row_count) / row_count
            part_cos = part_cos + round(math.cos(angle), 15) * wide[shift]
            part_sin = part_sin + round(math.sin(angle), 15) * wide[shift]
        twist = (high * local_pos % seq_len).astype(jnp.float32) * (2.0 * math.pi / seq_len)
        twist_cos = jnp.cos(twist)[:, None]
        twist_sin = jnp.sin(twist)[:, None]
        real = part_cos * twist_cos + part_sin * twist_sin
        imag = part_sin * twist_cos - part_cos * twist_sin
        reals.append(jnp.where(takes_sine, -imag, real).astype(jnp.bfloat16))
        imags.append(jnp.where(takes_sine, real, imag).astype(jnp.bfloat16))
    stacked = jnp.concatenate(
        [jnp.concatenate(reals, axis=1), jnp.concatenate(imags, axis=1)], axis=0
    )
    low_idx = jnp.arange(block_len, dtype=jnp.int32)
    low_cos, low_sin = phases(low_idx, low_idx, block_len)
    low_table = jnp.concatenate([low_cos, low_sin], 1) / math.sqrt(seq_len)
    spectrum = jnp.dot(
        low_table.astype(jnp.bfloat16), stacked, preferred_element_type=jnp.float32
    ).astype(jnp.bfloat16)
    spectrum = spectrum.reshape(row_count, low_len, row_count * slab)
    back = [to_row(spectrum, 0)]
    for shift in range(1, row_count):
        back.append(along_row(to_row(spectrum, shift), shift))
    own = jnp.stack(back)

    fold = folding_matrix(row_index, row_count, width)
    weights = []
    for flip in range(col_count):
        rows = lax.dynamic_slice(out_weight, ((col_index ^ flip) * width, 0), (width, width))
        weights.append(
            jnp.dot(fold, rows, preferred_element_type=jnp.float32).astype(jnp.bfloat16)
        )

    next_x = across_col(own, 1)
    next_y = across_col(own, 2)
    cut = row_count // 2
    far = jnp.concatenate([across_col(next_y[:cut], 1), across_col(next_x[cut:], 2)], 0)
    mixed = 0.0
    for part, weight in zip((own, next_x, next_y, far), weights):
        part = part.reshape(row_count, low_len, row_count, slab)
        part = part.transpose(1, 2, 0, 3).reshape(block_len, width)
        mixed = mixed + jnp.dot(part, weight, preferred_element_type=jnp.float32)
    return mixed.astype(jnp.bfloat16)


def solution(mesh):
    placed = (P("row", "col"), P(), P(None, "col"))
    whole_groups = mesh.shape["col"] == GROUPS == 4
    body = on_device_whole_groups if whole_groups else on_device
    return jax.shard_map(
        body, mesh=mesh, in_specs=placed, out_specs=P("row", "col"), check_vma=False
    )
```

```python
import functools
import math

import jax
import jax.numpy as jnp
from jax import lax
from jax.experimental import pallas as pl
from jax.experimental.pallas import tpu as pltpu
from jax.sharding import PartitionSpec as P

GROUPS = 4


EPSILON = 1e-06
PRECISE = lax.Precision.HIGHEST


def phases(left_idx, right_idx, period):
    product = left_idx[:, None] * right_idx[None, :] % period
    angles = product.astype(jnp.float32) * (2.0 * math.pi / period)
    return (jnp.cos(angles), jnp.sin(angles))


def split_table(table):
    table_high = table.astype(jnp.bfloat16)
    remainder = table - table_high.astype(jnp.float32)
    table_middle = remainder.astype(jnp.bfloat16)
    table_low = (remainder - table_middle.astype(jnp.float32)).astype(jnp.bfloat16)
    return (table_high, table_middle, table_low)


def on_device(tokens, norm_gain, out_weight):
    row_count = lax.axis_size("row")
    col_count = lax.axis_size("col")
    block_len, local_width = tokens.shape
    full_width = local_width * col_count
    group_len = full_width // GROUPS
    share_len = block_len // col_count
    seq_len = block_len * row_count
    slab_len = full_width // row_count
    col_index = lax.axis_index("col")
    chan_idx = jnp.arange(group_len, dtype=jnp.int32)
    cosines, sines = phases(chan_idx, chan_idx, group_len)
    chan_table = jnp.concatenate([cosines, sines], axis=1) / math.sqrt(group_len)
    table_parts = split_table(chan_table)
    arranged = tokens.reshape(col_count, share_len, local_width)
    portion = lax.all_to_all(arranged, "col", split_axis=0, concat_axis=2, tiled=True)
    item_count = portion.shape[1]
    values = portion.astype(jnp.float32)
    inv_rms = lax.rsqrt(jnp.mean(values * values, axis=-1, keepdims=True) + EPSILON)
    normed = lax.optimization_barrier((values * inv_rms * norm_gain).astype(jnp.bfloat16))
    grouped = normed.reshape(item_count, GROUPS, group_len)
    result = jnp.einsum("pgm,mj->pgj", grouped, table_parts[0], preferred_element_type=jnp.float32)
    result = result + jnp.einsum(
        "pgm,mj->pgj", grouped, table_parts[1], preferred_element_type=jnp.float32
    )
    result = result + jnp.einsum(
        "pgm,mj->pgj", grouped, table_parts[2], preferred_element_type=jnp.float32
    )
    high_idx = jnp.arange(row_count, dtype=jnp.int32)
    high_cos, high_sin = phases(high_idx, high_idx, row_count)
    high_table = jnp.concatenate(
        [jnp.concatenate([high_cos, -high_sin], 1), jnp.concatenate([-high_sin, -high_cos], 1)], 0
    )
    parts = (
        lax.all_to_all(
            result[..., :group_len].reshape(1, item_count, full_width),
            "row",
            split_axis=2,
            concat_axis=0,
            tiled=True,
        ),
        lax.all_to_all(
            result[..., group_len:].reshape(1, item_count, full_width),
            "row",
            split_axis=2,
            concat_axis=0,
            tiled=True,
        ),
    )
    item_count = parts[0].shape[1]
    stacked = jnp.concatenate(parts, 0).reshape(2 * row_count, item_count * slab_len)
    result = jnp.dot(high_table, stacked, precision=PRECISE)
    real_part = result[:row_count].reshape(row_count, item_count, slab_len)
    imag_part = result[row_count:].reshape(row_count, item_count, slab_len)
    local_pos = col_index * share_len + jnp.arange(share_len, dtype=jnp.int32)
    twist_cos, twist_sin = phases(high_idx, local_pos, seq_len)
    twist_cos = twist_cos[:, :, None]
    twist_sin = twist_sin[:, :, None]
    turned_real = real_part * twist_cos + imag_part * twist_sin
    turned_imag = imag_part * twist_cos - real_part * twist_sin
    low_idx = jnp.arange(block_len, dtype=jnp.int32)
    low_cos, low_sin = phases(low_idx, low_idx, block_len)
    low_cos = low_cos / math.sqrt(seq_len)
    low_sin = low_sin / math.sqrt(seq_len)
    low_table = jnp.concatenate([low_cos, low_sin], 1)
    stacked = jnp.concatenate(
        (
            lax.all_to_all(turned_real, "col", split_axis=0, concat_axis=1, tiled=True),
            lax.all_to_all(turned_imag, "col", split_axis=0, concat_axis=1, tiled=True),
        ),
        1,
    )
    finished = (jnp.einsum("ks,asc->akc", low_table, stacked, precision=PRECISE),)[0]
    spectrum = finished.astype(jnp.bfloat16)
    returned = lax.all_to_all(spectrum, "row", split_axis=1, concat_axis=2, tiled=True)
    mapped = jnp.einsum(
        "akd,de->kae",
        lax.all_gather(returned, "col", axis=0, tiled=True),
        out_weight,
        preferred_element_type=jnp.float32,
    )
    return mapped.astype(jnp.bfloat16).reshape(block_len, local_width)


def cosine_turns(index, period, quarter=0.0):
    turns = index.astype(jnp.float32) * (1.0 / period) - 0.25 * quarter
    turns = jnp.abs(turns - jnp.round(turns))
    angle = (0.25 - turns) * (2.0 * math.pi)
    square = angle * angle
    series = 1.0 / math.factorial(13)
    for order in (11, 9, 7, 5, 3, 1):
        sign = 1.0 if order % 4 == 1 else -1.0
        series = series * square + sign / math.factorial(order)
    return angle * series


def wrapped(index, period):
    if period & (period - 1) == 0:
        return index & (period - 1)
    return index % period


def channel_body(place_ref, tokens_ref, gain_ref, out_ref, table_ref):
    row_count, block_len, slab = out_ref.shape
    width = row_count * slab
    half = slab // 2
    fine_len = 1 << (width.bit_length() // 2)
    lane = lax.broadcasted_iota(jnp.int32, (fine_len, width), 1)
    step = lax.broadcasted_iota(jnp.int32, (fine_len, width), 0)
    in_slab = wrapped(lane, slab)
    is_sine = in_slab >= half
    freq = (lane - in_slab) // 2 + jnp.where(is_sine, in_slab - half, in_slab)
    packed = is_sine & (freq == 0)
    freq = jnp.where(packed, width // 2, freq)
    quarter = jnp.where(is_sine & ~packed, 1.0, 0.0)
    scale = 1.0 / math.sqrt(width)
    fine = wrapped(step * freq, width)
    fine_cos = cosine_turns(fine, width, quarter) * scale
    fine_sin = cosine_turns(fine, width, quarter + 1.0) * scale
    coarse = wrapped(step * fine_len * freq, width)
    coarse_cos = cosine_turns(coarse, width)
    coarse_sin = cosine_turns(coarse, width, 1.0)
    for start in range(width // fine_len):
        rows = coarse_cos[start : start + 1] * fine_cos - coarse_sin[start : start + 1] * fine_sin
        table_ref[start * fine_len : (start + 1) * fine_len, :] = rows.astype(jnp.bfloat16)
    gained = (tokens_ref[...].astype(jnp.float32) * gain_ref[...]).astype(jnp.bfloat16)
    for begin in range(0, row_count, 2):
        result = jnp.dot(
            gained,
            table_ref[:, begin * slab : (begin + 2) * slab],
            preferred_element_type=jnp.float32,
        )
        for row in range(begin, begin + 2):
            shift = lax.rem(row - place_ref[0] + row_count, row_count)
            out_ref[shift] = result[:, (row - begin) * slab : (row - begin + 1) * slab]


def sequence_body(place_ref, *refs):
    row_count, block_len, slab = refs[-3].shape
    got_refs = refs[:row_count]
    straight_ref, crossed_ref, low_ref, out_ref, stacked_ref, natural_ref = refs[row_count:]
    chunk = 32

    def spread(step, carry):
        rows = pl.ds(pl.multiple_of(step * chunk, chunk), chunk)
        imag_rows = pl.ds(pl.multiple_of(block_len + step * chunk, chunk), chunk)
        wide = [ref[rows, :].astype(jnp.float32) for ref in got_refs]
        evens, odds = [wide[0]], [None]
        for shift in range(1, (row_count + 1) // 2):
            evens.append(wide[shift] + wide[row_count - shift])
            odds.append(wide[shift] - wide[row_count - shift])
        if row_count % 2 == 0:
            evens.append(wide[row_count // 2])
            odds.append(None)
        for high in range(row_count // 2 + 1):
            part_cos = None
            part_sin = None
            for shift in range(len(evens)):
                angle = 2.0 * math.pi * (shift * high % row_count) / row_count
                weight = round(math.cos(angle), 15)
                if weight != 0.0:
                    term = evens[shift] if abs(weight) == 1.0 else evens[shift] * abs(weight)
                    if part_cos is None:
                        part_cos = term if weight > 0 else -term
                    else:
                        part_cos = part_cos + term if weight > 0 else part_cos - term
                weight = round(math.sin(angle), 15)
                if weight != 0.0 and odds[shift] is not None:
                    term = odds[shift] if abs(weight) == 1.0 else odds[shift] * abs(weight)
                    if part_sin is None:
                        part_sin = term if weight > 0 else -term
                    else:
                        part_sin = part_sin + term if weight > 0 else part_sin - term
            for target in {high, (row_count - high) % row_count}:
                straight = straight_ref[target, rows, :]
                crossed = crossed_ref[target, rows, :]
                upper = part_cos * straight
                lower = -(part_cos * crossed)
                if part_sin is not None:
                    turned = part_sin if target == high else -part_sin
                    upper = upper + turned * crossed
                    lower = lower + turned * straight
                lanes = slice(target * slab, (target + 1) * slab)
                stacked_ref[rows, lanes] = upper.astype(jnp.bfloat16)
                stacked_ref[imag_rows, lanes] = lower.astype(jnp.bfloat16)
        return carry

    lax.fori_loop(0, block_len // chunk, spread, 0)
    for begin in range(0, row_count, 2):
        result = jnp.dot(
            low_ref[...],
            stacked_ref[:, begin * slab : (begin + 2) * slab],
            preferred_element_type=jnp.float32,
        )
        for high in range(begin, begin + 2):
            natural_ref[pl.ds(high, block_len, row_count), :] = result[
                :, (high - begin) * slab : (high - begin + 1) * slab
            ]
    for row in range(row_count):
        shift = lax.rem(row - place_ref[0] + row_count, row_count)
        out_ref[shift] = natural_ref[row * block_len : (row + 1) * block_len, :].astype(jnp.bfloat16)


def folding_body(place_ref, weight_ref, out_ref, fold_ref, *, slab):
    width = fold_ref.shape[0]
    row_count = width // slab
    half = slab // 2

    @pl.when(pl.program_id(0) == 0)
    def _():
        out_idx = lax.broadcasted_iota(jnp.int32, (width, 1), 0)
        in_slab = wrapped(out_idx, slab)
        source = wrapped(place_ref[0] - out_idx // slab + row_count, row_count)
        is_sine = in_slab >= half
        freq = source * half + jnp.where(is_sine, in_slab - half, in_slab)
        packed = is_sine & (freq == 0)
        freq = jnp.where(packed, width // 2, freq)
        sign = jnp.where(is_sine & ~packed, -1.0, 1.0)
        chan = lax.broadcasted_iota(jnp.int32, (width, width), 1)
        other = wrapped(width - freq, width)
        straight = jnp.where(chan == freq, sign, 0.0)
        mirrored = jnp.where((chan == other) & (chan != freq), 1.0, 0.0)
        fold_ref[...] = (straight + mirrored).astype(jnp.bfloat16)

    out_ref[0] = jnp.dot(
        fold_ref[...], weight_ref[...], preferred_element_type=jnp.float32
    ).astype(jnp.bfloat16)


def mixing_body(*refs, piece_count, has_carry):
    pieces = [refs[k][...] for k in range(piece_count)]
    weight_ref = refs[piece_count]
    out_ref = refs[-1]
    left = jnp.concatenate(pieces, axis=1)
    right = weight_ref[...].reshape(left.shape[1], out_ref.shape[1])
    result = jnp.dot(left, right, preferred_element_type=jnp.float32)
    if has_carry:
        result = result + refs[piece_count + 1][...]
    out_ref[...] = result.astype(out_ref.dtype)


def in_vmem():
    return pl.BlockSpec(memory_space=pltpu.VMEM)


def in_smem():
    return pl.BlockSpec(memory_space=pltpu.SMEM)


def on_device_whole_groups(tokens, norm_gain, out_weight):
    row_count = lax.axis_size("row")
    col_count = lax.axis_size("col")
    block_len, width = tokens.shape
    full_width = width * col_count
    out_width = out_weight.shape[1]
    slab = width // row_count
    half = slab // 2
    seq_len = block_len * row_count
    row_index = lax.axis_index("row")
    col_index = lax.axis_index("col")
    place = jnp.stack([row_index, col_index]).astype(jnp.int32)

    def across_col(value, flip):
        return lax.ppermute(value, "col", [(k, k ^ flip) for k in range(col_count)])

    def along_row(value, shift):
        return lax.ppermute(
            value, "row", [(k, (k + shift) % row_count) for k in range(row_count)]
        )

    values = tokens.astype(jnp.float32)
    squares = jnp.sum(values * values, axis=-1)
    total = squares
    for flip in range(1, col_count):
        total = total + across_col(squares, flip)
    inv_rms = lax.rsqrt(total / full_width + EPSILON)
    gain = lax.dynamic_slice(norm_gain, (col_index * width,), (width,))
    chan = pl.pallas_call(
        channel_body,
        out_shape=jax.ShapeDtypeStruct((row_count, block_len, slab), jnp.float32),
        in_specs=[in_smem(), in_vmem(), in_vmem()],
        out_specs=in_vmem(),
        scratch_shapes=[pltpu.VMEM((width, width), jnp.bfloat16)],
        cost_estimate=pl.CostEstimate(
            flops=2 * block_len * width * width, transcendentals=0, bytes_accessed=4 * block_len * width
        ),
        name="channel_transform",
    )(place, tokens, gain[None, :])
    chan = (chan * inv_rms[None, :, None]).astype(jnp.bfloat16)

    got = [chan[0]]
    for shift in range(1, row_count):
        got.append(along_row(chan[shift], shift))

    local_pos = row_index * block_len + jnp.arange(block_len, dtype=jnp.int32)
    lane = jnp.arange(slab, dtype=jnp.int32)
    takes_sine = (lane >= half) & ~((lane == half) & (row_index == 0))
    high_idx = jnp.arange(row_count, dtype=jnp.int32)
    twist = wrapped(high_idx[:, None] * local_pos[None, :], seq_len)
    twist_cos = cosine_turns(twist, seq_len)[:, :, None]
    twist_sin = cosine_turns(twist, seq_len, 1.0)[:, :, None]
    straight = jnp.where(takes_sine, twist_sin, twist_cos)
    crossed = jnp.where(takes_sine, -twist_cos, twist_sin)
    low_idx = jnp.arange(block_len, dtype=jnp.int32)
    low_prod = wrapped(low_idx[:, None] * low_idx[None, :], block_len)
    low_table = jnp.concatenate(
        [cosine_turns(low_prod, block_len), cosine_turns(low_prod, block_len, 1.0)], 1
    )
    low_table = (low_table / math.sqrt(seq_len)).astype(jnp.bfloat16)

    weights = pl.pallas_call(
        functools.partial(folding_body, slab=slab),
        out_shape=jax.ShapeDtypeStruct((col_count, width, out_width), jnp.bfloat16),
        grid_spec=pltpu.PrefetchScalarGridSpec(
            num_scalar_prefetch=1,
            grid=(col_count,),
            in_specs=[pl.BlockSpec((width, out_width), lambda p, place: (place[1] ^ p, 0))],
            out_specs=pl.BlockSpec((1, width, out_width), lambda p, place: (p, 0, 0)),
            scratch_shapes=[pltpu.VMEM((width, width), jnp.bfloat16)],
        ),
        cost_estimate=pl.CostEstimate(
            flops=2 * col_count * width * width * out_width,
            transcendentals=0,
            bytes_accessed=4 * col_count * width * out_width,
        ),
        name="fold_weights",
    )(place, out_weight)

    spectrum = pl.pallas_call(
        sequence_body,
        out_shape=jax.ShapeDtypeStruct((row_count, block_len, slab), jnp.bfloat16),
        in_specs=[in_smem()] + [in_vmem()] * (row_count + 3),
        out_specs=in_vmem(),
        scratch_shapes=[
            pltpu.VMEM((2 * block_len, width), jnp.bfloat16),
            pltpu.VMEM((seq_len, slab), jnp.float32),
        ],
        cost_estimate=pl.CostEstimate(
            flops=4 * block_len * block_len * width, transcendentals=0, bytes_accessed=10 * block_len * width
        ),
        name="sequence_transform",
    )(place, *got, straight, crossed, low_table)

    back = [spectrum[0]]
    for shift in range(1, row_count):
        back.append(along_row(spectrum[shift], shift))

    group = 2
    mixed = None
    for begin in range(0, row_count, group):
        own = jnp.stack(back[begin : begin + group])
        next_x = across_col(own, 1)
        next_y = across_col(own, 2)
        cut = group // 2
        far_x = across_col(next_y[:cut], 1)
        far_y = across_col(next_x[cut:], 2)
        pieces = [part[k] for part in (own, next_x, next_y, far_x, far_y) for k in range(part.shape[0])]
        last = begin + group >= row_count
        part_rows = weights.reshape(col_count, row_count // group, group * slab, out_width)
        args = pieces + [part_rows[:, begin // group]] + ([] if mixed is None else [mixed])
        mixed = pl.pallas_call(
            functools.partial(
                mixing_body, piece_count=len(pieces), has_carry=mixed is not None
            ),
            out_shape=jax.ShapeDtypeStruct(
                (block_len, out_width), jnp.bfloat16 if last else jnp.float32
            ),
            in_specs=[in_vmem()] * len(args),
            out_specs=in_vmem(),
            cost_estimate=pl.CostEstimate(
                flops=2 * block_len * col_count * group * slab * out_width,
                transcendentals=0,
                bytes_accessed=8 * block_len * out_width,
            ),
            name="mix_channels",
        )(*args)
    return mixed


def solution(mesh):
    placed = (P("row", "col"), P(), P(None, "col"))
    whole_groups = mesh.shape["col"] == GROUPS == 4 and mesh.shape["row"] % 2 == 0
    body = on_device_whole_groups if whole_groups else on_device
    return jax.shard_map(
        body, mesh=mesh, in_specs=placed, out_specs=P("row", "col"), check_vma=False
    )
```
